32 devices in a mesh: tp: 8 (over z, y), dp: 4 (over x, core).
Axes of the slice: x: 2, y: 2, z: 4, core: 2. Of those that a mesh axis runs over, the one named last changes fastest.
Arguments:
- stream: bfloat16 [256, 2048], P('tp', 'dp'), may hold values from -12 to 12
- norm_gain: float32 [2, 2048], P(None, 'dp'), may hold values from 0.1 to 1.9
- w_input: bfloat16 [2, 2048, 2048], P(None, 'dp', 'tp'), may hold values from -0.125 to 0.125
- lam_re: float32 [2, 128, 64], P(None, 'tp'), may hold values from -1 to -0.05
- lam_im: float32 [2, 128, 64], P(None, 'tp'), may hold values from 0 to 6
- log_dt: float32 [2, 128], P(None, 'tp'), may hold values from -3 to 0
- b_re: float32 [2, 128, 64, 16], P(None, 'tp'), may hold values from -1 to 1
- b_im: float32 [2, 128, 64, 16], P(None, 'tp'), may hold values from -1 to 1
- readout_real: float32 [2, 128, 16, 64], P(None, 'tp'), may hold values from -0.5 to 0.5
- readout_imaginary: float32 [2, 128, 16, 64], P(None, 'tp'), may hold values from -0.5 to 0.5
- d_skip: float32 [2, 2048], P(None, 'tp'), may hold values from -4 to 4
- w_val: bfloat16 [2, 2048, 2048], P(None, 'tp', 'dp'), may hold values from -0.375 to 0.375
- w_gate: bfloat16 [2, 2048, 2048], P(None, 'tp', 'dp'), may hold values from -0.375 to 0.375
- state: float32 [2, 256, 128, 128], P(None, 'dp', 'tp'), may hold values from -6 to 6
Outputs:
- stream_out: bfloat16 [256, 2048], P('tp', 'dp')
- states_out: float32 [2, 256, 128, 128], P(None, 'dp', 'tp')
The draws below stay inside these ranges and needn't reach their ends.
All inputs are finite; a program needn't handle non-finite values.
Results may differ from the reference program's by a relative error of at most 0.0064.
Values may be sent and summed in bfloat16 or wider, within the bound.
A program may use at most 64 MiB of HBM per device.

```python
import jax
import jax.numpy as jnp
from jax import lax

D = 2048
CH = 16
STATE = 64
GROUPS = 128
LAYERS = 2
SEQS = 256


def draw_stream(key, part):
    subkeys = jax.random.split(key, 2)
    base_draw = jax.random.normal(subkeys[0], (SEQS, D), jnp.float32)
    block_scale = jnp.exp(jax.random.uniform(subkeys[1], (SEQS, 8), jnp.float32, -1.2, 1.2))
    full_draw = base_draw * jnp.repeat(block_scale, D // 8, axis=1)
    return jnp.clip(full_draw, -12.0, 12.0).astype(jnp.bfloat16)


def level_of(rng, extent, cuts, low, largest):
    loudness, own = 1.0, jax.random.fold_in(rng, 6)
    for dim, shards_of in cuts:
        heights = jnp.exp(jax.random.uniform(jax.random.fold_in(own, dim), (shards_of,), jnp.float32, low / len(cuts), largest / len(cuts)))
        loudness = loudness * jnp.repeat(heights, extent[dim] // shards_of).reshape([-1 if axis == dim else 1 for axis in range(len(extent))])
    return loudness


def bell_draw(rng, shape, scale, limit, cuts=(), held_as=jnp.bfloat16):
    result = scale * jax.random.normal(rng, shape, jnp.float32)
    if cuts:
        result = result * level_of(rng, shape, cuts, -0.22, 0.18)
    return jnp.clip(result, -limit, limit).astype(held_as)


def setup_inputs(seed: int = 0) -> dict:
    keys = jax.random.split(jax.random.key(seed), 15)
    stream = draw_stream(jax.random.fold_in(keys[14], 71), 0)
    norm_gain = jnp.clip(1.0 + 0.18 * jax.random.normal(keys[1], (LAYERS, D), jnp.float32), 0.1, 1.9)
    w_input = bell_draw(keys[2], (LAYERS, D, D), D ** -0.5, 0.125, ((1, 4), (2, 8)))
    lam_re = jnp.clip(-1.0 + 0.95 * jax.random.uniform(keys[3], (LAYERS, GROUPS, STATE), jnp.float32) ** level_of(keys[3], (LAYERS, GROUPS, STATE), ((1, 8),), -0.2, 0.2), -1.0, -0.05)
    lam_im = jnp.clip(6.0 * jax.random.uniform(keys[4], (LAYERS, GROUPS, STATE), jnp.float32) ** level_of(keys[4], (LAYERS, GROUPS, STATE), ((1, 8),), -0.2, 0.2), 0.0, 6.0)
    log_dt = jnp.clip(-3.0 + 3.0 * jax.random.uniform(keys[5], (LAYERS, GROUPS), jnp.float32) ** level_of(keys[5], (LAYERS, GROUPS), ((1, 8),), -0.2, 0.2), -3.0, 0.0)
    b_re = bell_draw(keys[6], (LAYERS, GROUPS, STATE, CH), (2 * CH) ** -0.5, 1.0, ((1, 8),), jnp.float32)
    b_im = bell_draw(keys[7], (LAYERS, GROUPS, STATE, CH), (2 * CH) ** -0.5, 1.0, ((1, 8),), jnp.float32)
    readout_real = bell_draw(keys[8], (LAYERS, GROUPS, CH, STATE), (2 * STATE) ** -0.5, 0.5, ((1, 8),), jnp.float32)
    readout_imaginary = bell_draw(keys[9], (LAYERS, GROUPS, CH, STATE), (2 * STATE) ** -0.5, 0.5, ((1, 8),), jnp.float32)
    d_skip = bell_draw(keys[10], (LAYERS, D), 1.0, 4.0, ((1, 8),), jnp.float32)
    w_val = bell_draw(keys[11], (LAYERS, D, D), (D // 8) ** -0.5, 0.375, ((1, 8), (2, 4)))
    w_gate = bell_draw(keys[12], (LAYERS, D, D), (D // 8) ** -0.5, 0.375, ((1, 8), (2, 4)))
    state = bell_draw(keys[13], (LAYERS, SEQS, GROUPS, 2 * STATE), 1.0, 6.0, ((1, 4), (2, 8)), jnp.float32)
    return {"stream": stream, "norm_gain": norm_gain, "w_input": w_input, "lam_re": lam_re, "lam_im": lam_im, "log_dt": log_dt, "b_re": b_re, "b_im": b_im, "readout_real": readout_real, "readout_imaginary": readout_imaginary, "d_skip": d_skip, "w_val": w_val, "w_gate": w_gate, "state": state}


eps = 1e-06

def advance(inputs, old_state, lam_re, lam_im, log_dt, b_re, b_im, readout_real, readout_imaginary, d_skip):
    upper_bound = lax.Precision.HIGHEST
    count_rows, groups, doubled = old_state.shape
    half_state = doubled // 2
    chans = b_re.shape[-1]
    step_size = jnp.exp(log_dt)[:, None]
    decay = jnp.exp(lam_re * step_size)
    angle = lam_im * step_size
    keep_re = decay * jnp.cos(angle)
    keep_im = decay * jnp.sin(angle)
    denom = lam_re * lam_re + lam_im * lam_im
    ratio_re = ((keep_re - 1.0) * lam_re + keep_im * lam_im) / denom
    ratio_im = (keep_im * lam_re - (keep_re - 1.0) * lam_im) / denom
    drive_re = ratio_re[..., None] * b_re - ratio_im[..., None] * b_im
    drive_im = ratio_re[..., None] * b_im + ratio_im[..., None] * b_re
    grouped = inputs.reshape(count_rows, groups, chans)
    push_re = jnp.einsum('gpc,rgc->rgp', drive_re, grouped, precision=upper_bound)
    push_im = jnp.einsum('gpc,rgc->rgp', drive_im, grouped, precision=upper_bound)
    old_re = old_state[..., :half_state]
    old_im = old_state[..., half_state:]
    updated_real = keep_re * old_re - keep_im * old_im + push_re
    updated_imaginary = keep_re * old_im + keep_im * old_re + push_im
    readout_output = jnp.einsum('aot,mat->mao', readout_real, updated_real, precision=upper_bound) - jnp.einsum('aot,mat->mao', readout_imaginary, updated_imaginary, precision=upper_bound)
    pre_act = readout_output.reshape(count_rows, groups * chans) + d_skip * inputs
    return (pre_act, jnp.concatenate([updated_real, updated_imaginary], axis=-1))

def reference(stream, norm_gain, w_input, lam_re, lam_im, log_dt, b_re, b_im, readout_real, readout_imaginary, d_skip, w_val, w_gate, state):
    collected = []
    for layer_no in range(LAYERS):
        widened = stream.astype(jnp.float32)
        factor = lax.rsqrt(lax.optimization_barrier(jnp.mean(widened * widened, axis=1)) + eps)
        normed = (widened * norm_gain[layer_no]).astype(jnp.bfloat16)
        inputs = factor[:, None] * jnp.dot(normed, w_input[layer_no], preferred_element_type=jnp.float32)
        pre_act, new_state = advance(inputs, state[layer_no], lam_re[layer_no], lam_im[layer_no], log_dt[layer_no], b_re[layer_no], b_im[layer_no], readout_real[layer_no], readout_imaginary[layer_no], d_skip[layer_no])
        mixed = jax.nn.gelu(pre_act).astype(jnp.bfloat16)
        value = jnp.dot(mixed, w_val[layer_no], preferred_element_type=jnp.float32)
        gate = jnp.dot(mixed, w_gate[layer_no], preferred_element_type=jnp.float32)
        stream = (widened + value * jax.nn.sigmoid(gate)).astype(jnp.bfloat16)
        collected.append(new_state)
    return (stream, jnp.stack(collected))
```

```python
import functools

import jax
import jax.numpy as jnp
from jax import lax
from jax.experimental import pallas as pl
from jax.experimental.pallas import tpu as pltpu
from jax.sharding import PartitionSpec as P

EPS = 1e-06
F32 = jnp.float32
BF16 = jnp.bfloat16
HIGHEST = lax.Precision.HIGHEST
NT = (((1,), (1,)), ((), ()))


def partner(me, k, n, back=False):
    if n & (n - 1):
        return (me + (n - k if back else k)) % n
    found, bit = 0, 1
    while bit < n:
        mine = (me // bit) % 2
        found = found + (bit * (1 - mine) if k & bit else bit * mine)
        bit *= 2
    return found


def kernel(
    tp, dp, chans,
    stream_ref, gain_ref, w_in_hbm, keep_ref, drive_hbm, read_hbm, skip_ref, w_val_hbm, w_gate_hbm, state_hbm,
    out_ref, states_hbm,
    w_in, w_val, w_gate, drive, read, state,
    kept, proj, u_keep, masked, from_old, mix_w,
    x_all, part_send, part_recv, sq_send, sq_recv, mix_all, comb_send, comb_own, comb_recv,
    load_sem, store_sem, x_ss, x_rs, part_ss, part_rs, sq_ss, sq_rs, mix_ss, mix_rs, comb_ss, comb_rs,
):
    layers = w_in.shape[0]
    me_t, me_d = lax.axis_index("tp"), lax.axis_index("dp")
    rows_t, feats = stream_ref.shape
    rows_d, width = u_keep.shape[1:]
    per = rows_d // rows_t
    groups = keep_ref.shape[2]
    lanes = state.shape[2]
    sq_width = sq_send.shape[3]

    loads = {}
    for l in range(layers):
        for i, (src, dst) in enumerate(
            ((state_hbm, state), (drive_hbm, drive), (read_hbm, read), (w_in_hbm, w_in), (w_val_hbm, w_val), (w_gate_hbm, w_gate))
        ):
            loads[l, i] = pltpu.make_async_copy(src.at[l], dst.at[l], load_sem.at[l, i])
            loads[l, i].start()

    barrier = pltpu.get_barrier_semaphore()
    for k in range(1, dp):
        pl.semaphore_signal(barrier, inc=1, device_id={"dp": partner(me_d, k, dp)}, device_id_type=pl.DeviceIdType.MESH)
    for k in range(1, tp):
        pl.semaphore_signal(barrier, inc=1, device_id={"tp": partner(me_t, k, tp)}, device_id_type=pl.DeviceIdType.MESH)

    def send(src, dst, ss, rs, axis, to):
        return pltpu.make_async_remote_copy(
            src_ref=src, dst_ref=dst, send_sem=ss, recv_sem=rs, device_id={axis: to}, device_id_type=pl.DeviceIdType.MESH
        )

    def x_copy(l, k):
        src = stream_ref if l == 0 else x_all.at[l, me_t]
        to = partner(me_t, k, tp)
        return send(src, x_all.at[l, me_t], x_ss.at[l, to], x_rs.at[l, me_t], "tp", to)

    def part_copy(l, to):
        return send(part_send.at[l, to], part_recv.at[l, me_d], part_ss.at[l, to], part_rs.at[l, me_d], "dp", to)

    def sq_copy(l, to):
        return send(sq_send.at[l, to], sq_recv.at[l, me_d], sq_ss.at[l, to], sq_rs.at[l, me_d], "dp", to)

    def mix_copy(l, to):
        return send(mix_all.at[l, me_d], mix_all.at[l, me_d], mix_ss.at[l, to], mix_rs.at[l, me_d], "dp", to)

    def comb_copy(l, to):
        return send(comb_send.at[l, to], comb_recv.at[l, me_t], comb_ss.at[l, to], comb_rs.at[l, me_t], "tp", to)

    def arrival(ref, rs, axis):
        return send(ref, ref, rs, rs, axis, 0)

    lane_group = lax.broadcasted_iota(jnp.int32, (rows_d, width), 1) // chans
    eye = lax.broadcasted_iota(jnp.int32, (rows_d, sq_width), 0) == lax.broadcasted_iota(jnp.int32, (rows_d, sq_width), 1)

    def prepare(l):
        for i in range(3):
            loads[l, i].wait()
        for g in range(groups):
            old = state[l, pl.ds(g, rows_d, stride=groups), :]
            kept[l, pl.ds(g * rows_d, rows_d), :] = (
                keep_ref[l, 0, g : g + 1, :] * old + keep_ref[l, 1, g : g + 1, :] * pltpu.roll(old, lanes // 2, 1)
            )
        proj[...] = lax.dot_general(kept[l], read[l], NT, precision=HIGHEST, preferred_element_type=F32)
        total = jnp.zeros((rows_d, width), F32)
        for g in range(groups):
            total = jnp.where(lane_group == g, proj[pl.ds(g * rows_d, rows_d), :], total)
        from_old[l] = total
        full = lax.dot_general(drive[l], read[l], NT, precision=HIGHEST, preferred_element_type=F32)
        same = (
            lax.broadcasted_iota(jnp.int32, (width, width), 0) // chans
            == lax.broadcasted_iota(jnp.int32, (width, width), 1) // chans
        )
        mix_w[l] = jnp.where(same, full, 0.0)

    def update(l):
        u = u_keep[l]
        for g in range(groups):
            masked[pl.ds(g * rows_d, rows_d), :] = jnp.where(lane_group == g, u, 0.0)
        kept[l] = kept[l] + jnp.dot(masked[...], drive[l], precision=HIGHEST, preferred_element_type=F32)
        for g in range(groups):
            state[l, pl.ds(g, rows_d, stride=groups), :] = kept[l, pl.ds(g * rows_d, rows_d), :]
        pltpu.make_async_copy(state.at[l], states_hbm.at[l], store_sem.at[l]).start()

    pl.semaphore_wait(barrier, tp + dp - 2)
    for k in reversed(range(1, tp)):
        x_copy(0, k).start()
    x_all[0, me_t] = stream_ref[...]
    prepare(0)

    for l in range(layers):
        loads[l, 3].wait()
        gain = gain_ref[l : l + 1, :]
        own_part = own_sq = None
        for k in reversed(range(dp)):
            to = partner(me_d, k, dp)
            for j in range(per):
                t = to * per + j

                @pl.when(t != me_t)
                def _():
                    arrival(x_all.at[l, t], x_rs.at[l, t], "tp").wait_recv()

            x = x_all[l, pl.ds(to * per, per)].astype(F32).reshape(rows_d, feats)
            column = jnp.sum(x * x, axis=1, keepdims=True)
            squares = jnp.sum(jnp.where(eye, column, 0.0), axis=0, keepdims=True)
            product = jnp.dot((x * gain).astype(BF16), w_in[l], preferred_element_type=F32)
            if k:
                sq_send[l, to] = jnp.broadcast_to(squares, (8, sq_width))
                sq_copy(l, to).start()
                part_send[l, to] = product.astype(BF16)
                part_copy(l, to).start()
            else:
                own_part, own_sq = product, squares
        for k in range(1, dp):
            by = partner(me_d, k, dp, True)
            arrival(sq_recv.at[l, by], sq_rs.at[l, by], "dp").wait_recv()
            own_sq = own_sq + sq_recv[l, by][0:1, :]
            arrival(part_recv.at[l, by], part_rs.at[l, by], "dp").wait_recv()
            own_part = own_part + part_recv[l, by].astype(F32)
        square_total = jnp.sum(jnp.where(eye, own_sq, 0.0), axis=1, keepdims=True)
        u = lax.rsqrt(square_total / (feats * dp) + EPS) * own_part
        u_keep[l] = u
        pre = from_old[l] + jnp.dot(u, mix_w[l], precision=HIGHEST, preferred_element_type=F32) + skip_ref[l : l + 1, :] * u
        mix_all[l, me_d] = jax.nn.gelu(pre).astype(BF16)
        for k in reversed(range(1, dp)):
            mix_copy(l, partner(me_d, k, dp)).start()
        loads[l, 4].wait()
        loads[l, 5].wait()
        for k in range(dp):
            by = partner(me_d, k, dp, True)
            if k:
                arrival(mix_all.at[l, by], mix_rs.at[l, by], "dp").wait_recv()
            mixed = mix_all[l, by]
            value = jnp.dot(mixed, w_val[l], preferred_element_type=F32)
            gate = jnp.dot(mixed, w_gate[l], preferred_element_type=F32)
            for j in range(per):
                t = by * per + j
                rows = slice(j * rows_t, (j + 1) * rows_t)

                @pl.when(t != me_t)
                def _():
                    comb_send[l, t, :, :feats] = value[rows].astype(BF16)
                    comb_send[l, t, :, feats:] = gate[rows].astype(BF16)
                    comb_copy(l, t).start()

                @pl.when(t == me_t)
                def _():
                    comb_own[:, :feats] = value[rows]
                    comb_own[:, feats:] = gate[rows]

        update(l)
        if l + 1 < layers:
            prepare(l + 1)
        combined = comb_own[...]
        for k in range(1, tp):
            by = partner(me_t, k, tp, True)
            arrival(comb_recv.at[l, by], comb_rs.at[l, by], "tp").wait_recv()
            combined = combined + comb_recv[l, by].astype(F32)
        fresh = (
            x_all[l, me_t].astype(F32) + combined[:, :feats] * jax.nn.sigmoid(combined[:, feats:])
        ).astype(BF16)
        if l + 1 < layers:
            x_all[l + 1, me_t] = fresh
            for k in reversed(range(1, tp)):
                x_copy(l + 1, k).start()
        else:
            out_ref[...] = fresh

    for l in range(layers):
        for k in range(1, tp):
            x_copy(l, k).wait_send()
            comb_copy(l, partner(me_t, k, tp)).wait_send()
        for k in range(1, dp):
            to = partner(me_d, k, dp)
            part_copy(l, to).wait_send()
            sq_copy(l, to).wait_send()
            mix_copy(l, to).wait_send()
        pltpu.make_async_copy(state.at[l], states_hbm.at[l], store_sem.at[l]).wait()


def per_device(
    tp, dp,
    stream, norm_gain, w_input, lam_re, lam_im, log_dt, b_re, b_im, readout_real, readout_imaginary, d_skip,
    w_val, w_gate, state,
):
    layers, feats, width = w_input.shape
    rows_t = stream.shape[0]
    rows_d, groups, lanes = state.shape[1:]
    chans = b_re.shape[-1]

    step_size = jnp.exp(log_dt)[..., None]
    decay = jnp.exp(lam_re * step_size)
    angle = lam_im * step_size
    keep_re = decay * jnp.cos(angle)
    keep_im = decay * jnp.sin(angle)
    denom = lam_re * lam_re + lam_im * lam_im
    ratio_re = (((keep_re - 1.0) * lam_re + keep_im * lam_im) / denom)[:, :, None, :]
    ratio_im = ((keep_im * lam_re - (keep_re - 1.0) * lam_im) / denom)[:, :, None, :]
    keep = jnp.stack(
        [jnp.concatenate([keep_re, keep_re], -1), jnp.concatenate([-keep_im, keep_im], -1)], axis=1
    )
    turned_re, turned_im = b_re.swapaxes(2, 3), b_im.swapaxes(2, 3)
    drive = jnp.concatenate(
        [ratio_re * turned_re - ratio_im * turned_im, ratio_re * turned_im + ratio_im * turned_re], -1
    ).reshape(layers, width, lanes)
    read = jnp.concatenate([readout_real, -readout_imaginary], -1).reshape(layers, width, lanes)

    vmem = pl.BlockSpec(memory_space=pltpu.VMEM)
    hbm = pl.BlockSpec(memory_space=pl.ANY)
    sq_width = max(rows_d, 128)
    dma = lambda *shape: pltpu.SemaphoreType.DMA(shape)
    out, states = pl.pallas_call(
        functools.partial(kernel, tp, dp, chans),
        out_shape=(
            jax.ShapeDtypeStruct(stream.shape, BF16),
            jax.ShapeDtypeStruct((layers, rows_d * groups, lanes), F32),
        ),
        in_specs=[vmem, vmem, hbm, vmem, hbm, hbm, vmem, hbm, hbm, hbm],
        out_specs=(vmem, hbm),
        scratch_shapes=[
            pltpu.VMEM(w_input.shape, BF16),
            pltpu.VMEM(w_val.shape, BF16),
            pltpu.VMEM(w_gate.shape, BF16),
            pltpu.VMEM(drive.shape, F32),
            pltpu.VMEM(read.shape, F32),
            pltpu.VMEM((layers, rows_d * groups, lanes), F32),
            pltpu.VMEM((layers, rows_d * groups, lanes), F32),
            pltpu.VMEM((rows_d * groups, width), F32),
            pltpu.VMEM((layers, rows_d, width), F32),
            pltpu.VMEM((rows_d * groups, width), F32),
            pltpu.VMEM((layers, rows_d, width), F32),
            pltpu.VMEM((layers, width, width), F32),
            pltpu.VMEM((layers, tp, rows_t, feats), BF16),
            pltpu.VMEM((layers, dp, rows_d, width), BF16),
            pltpu.VMEM((layers, dp, rows_d, width), BF16),
            pltpu.VMEM((layers, dp, 8, sq_width), F32),
            pltpu.VMEM((layers, dp, 8, sq_width), F32),
            pltpu.VMEM((layers, dp, rows_d, width), BF16),
            pltpu.VMEM((layers, tp, rows_t, 2 * feats), BF16),
            pltpu.VMEM((rows_t, 2 * feats), F32),
            pltpu.VMEM((layers, tp, rows_t, 2 * feats), BF16),
            dma(layers, 6), dma(layers),
            dma(layers, tp), dma(layers, tp),
            dma(layers, dp), dma(layers, dp),
            dma(layers, dp), dma(layers, dp),
            dma(layers, dp), dma(layers, dp),
            dma(layers, tp), dma(layers, tp),
        ],
        compiler_params=pltpu.CompilerParams(collective_id=0, has_side_effects=True, vmem_limit_bytes=56 * 1024 * 1024),
    )(
        stream, norm_gain, w_input, keep, drive, read, d_skip, w_val, w_gate,
        state.reshape(layers, rows_d * groups, lanes),
    )
    return out, states.reshape(state.shape)


def solution(mesh):
    return jax.shard_map(
        functools.partial(per_device, mesh.shape["tp"], mesh.shape["dp"]),
        mesh=mesh,
        in_specs=(
            P("tp", "dp"),
            P(None, "dp"),
            P(None, "dp", "tp"),
            P(None, "tp", None),
            P(None, "tp", None),
            P(None, "tp"),
            P(None, "tp", None, None),
            P(None, "tp", None, None),
            P(None, "tp", None, None),
            P(None, "tp", None, None),
            P(None, "tp"),
            P(None, "tp", "dp"),
            P(None, "tp", "dp"),
            P(None, "dp", "tp", None),
        ),
        out_specs=(P("tp", "dp"), P(None, "dp", "tp", None)),
        check_vma=False,
    )
```

```python
import functools

import jax
import jax.numpy as jnp
from jax import lax
from jax.experimental import pallas as pl
from jax.experimental.pallas import tpu as pltpu
from jax.sharding import PartitionSpec as P

EPS = 1e-06
F32 = jnp.float32
BF16 = jnp.bfloat16
HIGHEST = lax.Precision.HIGHEST
NT = (((1,), (1,)), ((), ()))


def partner(me, k, n, back=False):
    if n & (n - 1):
        return (me + (n - k if back else k)) % n
    found, bit = 0, 1
    while bit < n:
        mine = (me // bit) % 2
        found = found + (bit * (1 - mine) if k & bit else bit * mine)
        bit *= 2
    return found


def kernel(
    tp, dp, chans,
    stream_ref, gain_ref, w_in_hbm, lam_re_ref, lam_im_ref, log_dt_ref, b_re_hbm, b_im_hbm, c_re_hbm, c_im_hbm, skip_ref,
    w_val_hbm, w_gate_hbm, state_hbm,
    out_ref, state,
    w_in, w_val, w_gate, b_re, b_im, c_re, c_im, drive, read,
    kept, proj, u_keep, masked, from_old, mix_w,
    x_all, part_send, part_recv, sq_send, sq_recv, mix_all, comb_send, comb_own, comb_recv,
    load_sem, x_ss, x_rs, part_ss, part_rs, sq_ss, sq_rs, mix_ss, mix_rs, comb_ss, comb_rs,
):
    layers = w_in.shape[0]
    me_t, me_d = lax.axis_index("tp"), lax.axis_index("dp")
    rows_t, feats = stream_ref.shape
    rows_d, width = u_keep.shape[1:]
    per = rows_d // rows_t
    groups, half = lam_re_ref.shape[1:]
    lanes = state.shape[2]
    sq_width = sq_send.shape[3]

    loads = {}
    for l in range(layers):
        for i, (src, dst) in enumerate(
            (
                (b_re_hbm, b_re), (b_im_hbm, b_im), (c_re_hbm, c_re), (c_im_hbm, c_im), (state_hbm, state),
                (w_in_hbm, w_in), (w_val_hbm, w_val), (w_gate_hbm, w_gate),
            )
        ):
            loads[l, i] = pltpu.make_async_copy(src.at[l], dst.at[l], load_sem.at[l, i])
            loads[l, i].start()

    barrier = pltpu.get_barrier_semaphore()
    for k in range(1, dp):
        pl.semaphore_signal(barrier, inc=1, device_id={"dp": partner(me_d, k, dp)}, device_id_type=pl.DeviceIdType.MESH)
    for k in range(1, tp):
        pl.semaphore_signal(barrier, inc=1, device_id={"tp": partner(me_t, k, tp)}, device_id_type=pl.DeviceIdType.MESH)

    def send(src, dst, ss, rs, axis, to):
        return pltpu.make_async_remote_copy(
            src_ref=src, dst_ref=dst, send_sem=ss, recv_sem=rs, device_id={axis: to}, device_id_type=pl.DeviceIdType.MESH
        )

    def x_copy(l, k):
        src = stream_ref if l == 0 else x_all.at[l, me_t]
        to = partner(me_t, k, tp)
        return send(src, x_all.at[l, me_t], x_ss.at[l, to], x_rs.at[l, me_t], "tp", to)

    def part_copy(l, to):
        return send(part_send.at[l, to], part_recv.at[l, me_d], part_ss.at[l, to], part_rs.at[l, me_d], "dp", to)

    def sq_copy(l, to):
        return send(sq_send.at[l, to], sq_recv.at[l, me_d], sq_ss.at[l, to], sq_rs.at[l, me_d], "dp", to)

    def mix_copy(l, to):
        return send(mix_all.at[l, me_d], mix_all.at[l, me_d], mix_ss.at[l, to], mix_rs.at[l, me_d], "dp", to)

    def comb_copy(l, to):
        return send(comb_send.at[l, to], comb_recv.at[l, me_t], comb_ss.at[l, to], comb_rs.at[l, me_t], "tp", to)

    def arrival(ref, rs, axis):
        return send(ref, ref, rs, rs, axis, 0)

    lane_group = lax.broadcasted_iota(jnp.int32, (rows_d, width), 1) // chans
    eye = lax.broadcasted_iota(jnp.int32, (rows_d, sq_width), 0) == lax.broadcasted_iota(jnp.int32, (rows_d, sq_width), 1)

    group_eye = lax.broadcasted_iota(jnp.int32, (groups, groups), 0) == lax.broadcasted_iota(jnp.int32, (groups, groups), 1)

    def prepare(l):
        step_size = jnp.exp(jnp.sum(jnp.where(group_eye, log_dt_ref[l : l + 1, :], 0.0), axis=1, keepdims=True))
        lam_re, lam_im = lam_re_ref[l], lam_im_ref[l]
        decay = jnp.exp(lam_re * step_size)
        angle = lam_im * step_size
        keep_re = decay * jnp.cos(angle)
        keep_im = decay * jnp.sin(angle)
        denom = lam_re * lam_re + lam_im * lam_im
        ratio_re = ((keep_re - 1.0) * lam_re + keep_im * lam_im) / denom
        ratio_im = (keep_im * lam_re - (keep_re - 1.0) * lam_im) / denom
        keep_a = jnp.concatenate([keep_re, keep_re], axis=1)
        keep_b = jnp.concatenate([-keep_im, keep_im], axis=1)
        for i in range(5):
            loads[l, i].wait()
        for g in range(groups):
            t_re, t_im = b_re[l, g], b_im[l, g]
            r_re, r_im = ratio_re[g : g + 1, :], ratio_im[g : g + 1, :]
            drive[l, pl.ds(g * chans, chans), :] = jnp.concatenate(
                [r_re * t_re - r_im * t_im, r_re * t_im + r_im * t_re], axis=1
            )
        read[l] = jnp.concatenate([c_re[l].reshape(width, half), -c_im[l].reshape(width, half)], axis=1)
        for g in range(groups):
            old = state[l, pl.ds(g, rows_d, stride=groups), :]
            kept[l, pl.ds(g * rows_d, rows_d), :] = (
                keep_a[g : g + 1, :] * old + keep_b[g : g + 1, :] * pltpu.roll(old, lanes // 2, 1)
            )
        proj[...] = lax.dot_general(kept[l], read[l], NT, precision=HIGHEST, preferred_element_type=F32)
        total = jnp.zeros((rows_d, width), F32)
        for g in range(groups):
            total = jnp.where(lane_group == g, proj[pl.ds(g * rows_d, rows_d), :], total)
        from_old[l] = total
        full = lax.dot_general(drive[l], read[l], NT, precision=HIGHEST, preferred_element_type=F32)
        same = (
            lax.broadcasted_iota(jnp.int32, (width, width), 0) // chans
            == lax.broadcasted_iota(jnp.int32, (width, width), 1) // chans
        )
        mix_w[l] = jnp.where(same, full, 0.0)

    def update(l):
        u = u_keep[l]
        for g in range(groups):
            masked[pl.ds(g * rows_d, rows_d), :] = jnp.where(lane_group == g, u, 0.0)
        kept[l] = kept[l] + jnp.dot(masked[...], drive[l], precision=HIGHEST, preferred_element_type=F32)
        for g in range(groups):
            state[l, pl.ds(g, rows_d, stride=groups), :] = kept[l, pl.ds(g * rows_d, rows_d), :]

    pl.semaphore_wait(barrier, tp + dp - 2)
    for k in reversed(range(1, tp)):
        x_copy(0, k).start()
    x_all[0, me_t] = stream_ref[...]
    prepare(0)

    for l in range(layers):
        loads[l, 5].wait()
        gain = gain_ref[l : l + 1, :]
        own_part = own_sq = None
        for k in reversed(range(dp)):
            to = partner(me_d, k, dp)
            for j in range(per):
                t = to * per + j

                @pl.when(t != me_t)
                def _():
                    arrival(x_all.at[l, t], x_rs.at[l, t], "tp").wait_recv()

            x = x_all[l, pl.ds(to * per, per)].astype(F32).reshape(rows_d, feats)
            column = jnp.sum(x * x, axis=1, keepdims=True)
            squares = jnp.sum(jnp.where(eye, column, 0.0), axis=0, keepdims=True)
            product = jnp.dot((x * gain).astype(BF16), w_in[l], preferred_element_type=F32)
            if k:
                sq_send[l, to] = jnp.broadcast_to(squares, (8, sq_width))
                sq_copy(l, to).start()
                part_send[l, to] = product.astype(BF16)
                part_copy(l, to).start()
            else:
                own_part, own_sq = product, squares
        for k in range(1, dp):
            by = partner(me_d, k, dp, True)
            arrival(sq_recv.at[l, by], sq_rs.at[l, by], "dp").wait_recv()
            own_sq = own_sq + sq_recv[l, by][0:1, :]
            arrival(part_recv.at[l, by], part_rs.at[l, by], "dp").wait_recv()
            own_part = own_part + part_recv[l, by].astype(F32)
        square_total = jnp.sum(jnp.where(eye, own_sq, 0.0), axis=1, keepdims=True)
        u = lax.rsqrt(square_total / (feats * dp) + EPS) * own_part
        u_keep[l] = u
        pre = from_old[l] + jnp.dot(u, mix_w[l], precision=HIGHEST, preferred_element_type=F32) + skip_ref[l : l + 1, :] * u
        mix_all[l, me_d] = jax.nn.gelu(pre).astype(BF16)
        for k in reversed(range(1, dp)):
            mix_copy(l, partner(me_d, k, dp)).start()
        loads[l, 6].wait()
        loads[l, 7].wait()
        for k in range(dp):
            by = partner(me_d, k, dp, True)
            if k:
                arrival(mix_all.at[l, by], mix_rs.at[l, by], "dp").wait_recv()
            mixed = mix_all[l, by]
            value = jnp.dot(mixed, w_val[l], preferred_element_type=F32)
            gate = jnp.dot(mixed, w_gate[l], preferred_element_type=F32)
            for j in range(per):
                t = by * per + j
                rows = slice(j * rows_t, (j + 1) * rows_t)

                @pl.when(t != me_t)
                def _():
                    comb_send[l, t, :, :feats] = value[rows].astype(BF16)
                    comb_send[l, t, :, feats:] = gate[rows].astype(BF16)
                    comb_copy(l, t).start()

                @pl.when(t == me_t)
                def _():
                    comb_own[:, :feats] = value[rows]
                    comb_own[:, feats:] = gate[rows]

        update(l)
        if l + 1 < layers:
            prepare(l + 1)
        combined = comb_own[...]
        for k in range(1, tp):
            by = partner(me_t, k, tp, True)
            arrival(comb_recv.at[l, by], comb_rs.at[l, by], "tp").wait_recv()
            combined = combined + comb_recv[l, by].astype(F32)
        fresh = (
            x_all[l, me_t].astype(F32) + combined[:, :feats] * jax.nn.sigmoid(combined[:, feats:])
        ).astype(BF16)
        if l + 1 < layers:
            x_all[l + 1, me_t] = fresh
            for k in reversed(range(1, tp)):
                x_copy(l + 1, k).start()
        else:
            out_ref[...] = fresh

    for l in range(layers):
        for k in range(1, tp):
            x_copy(l, k).wait_send()
            comb_copy(l, partner(me_t, k, tp)).wait_send()
        for k in range(1, dp):
            to = partner(me_d, k, dp)
            part_copy(l, to).wait_send()
            sq_copy(l, to).wait_send()
            mix_copy(l, to).wait_send()


def per_device(
    tp, dp,
    stream, norm_gain, w_input, lam_re, lam_im, log_dt, b_re, b_im, readout_real, readout_imaginary, d_skip,
    w_val, w_gate, state,
):
    layers, feats, width = w_input.shape
    rows_t = stream.shape[0]
    rows_d, groups, lanes = state.shape[1:]
    chans = b_re.shape[-1]

    turned_re, turned_im = b_re.swapaxes(2, 3), b_im.swapaxes(2, 3)

    limit = 67043328 - 4 * layers * rows_d * groups * lanes - (256 << 10)
    vmem = pl.BlockSpec(memory_space=pltpu.VMEM)
    hbm = pl.BlockSpec(memory_space=pltpu.HBM)
    sq_width = max(rows_d, 128)
    dma = lambda *shape: pltpu.SemaphoreType.DMA(shape)
    out, states = pl.pallas_call(
        functools.partial(kernel, tp, dp, chans),
        out_shape=(pltpu.VMEM(stream.shape, BF16), pltpu.VMEM((layers, rows_d * groups, lanes), F32)),
        in_specs=[vmem, vmem, hbm, vmem, vmem, vmem, hbm, hbm, hbm, hbm, vmem, hbm, hbm, hbm],
        out_specs=(vmem, vmem),
        scratch_shapes=[
            pltpu.VMEM(w_input.shape, BF16),
            pltpu.VMEM(w_val.shape, BF16),
            pltpu.VMEM(w_gate.shape, BF16),
            pltpu.VMEM(turned_re.shape, F32),
            pltpu.VMEM(turned_im.shape, F32),
            pltpu.VMEM(readout_real.shape, F32),
            pltpu.VMEM(readout_imaginary.shape, F32),
            pltpu.VMEM((layers, width, lanes), F32),
            pltpu.VMEM((layers, width, lanes), F32),
            pltpu.VMEM((layers, rows_d * groups, lanes), F32),
            pltpu.VMEM((rows_d * groups, width), F32),
            pltpu.VMEM((layers, rows_d, width), F32),
            pltpu.VMEM((rows_d * groups, width), F32),
            pltpu.VMEM((layers, rows_d, width), F32),
            pltpu.VMEM((layers, width, width), F32),
            pltpu.VMEM((layers, tp, rows_t, feats), BF16),
            pltpu.VMEM((layers, dp, rows_d, width), BF16),
            pltpu.VMEM((layers, dp, rows_d, width), BF16),
            pltpu.VMEM((layers, dp, 8, sq_width), F32),
            pltpu.VMEM((layers, dp, 8, sq_width), F32),
            pltpu.VMEM((layers, dp, rows_d, width), BF16),
            pltpu.VMEM((layers, tp, rows_t, 2 * feats), BF16),
            pltpu.VMEM((rows_t, 2 * feats), F32),
            pltpu.VMEM((layers, tp, rows_t, 2 * feats), BF16),
            dma(layers, 8),
            dma(layers, tp), dma(layers, tp),
            dma(layers, dp), dma(layers, dp),
            dma(layers, dp), dma(layers, dp),
            dma(layers, dp), dma(layers, dp),
            dma(layers, tp), dma(layers, tp),
        ],
        compiler_params=pltpu.CompilerParams(collective_id=0, has_side_effects=True, vmem_limit_bytes=limit),
    )(
        stream, norm_gain, w_input, lam_re, lam_im, log_dt, turned_re, turned_im, readout_real,
        readout_imaginary, d_skip, w_val, w_gate,
        state.reshape(layers, rows_d * groups, lanes),
    )
    return out, states.reshape(state.shape)


def solution(mesh):
    return jax.shard_map(
        functools.partial(per_device, mesh.shape["tp"], mesh.shape["dp"]),
        mesh=mesh,
        in_specs=(
            P("tp", "dp"),
            P(None, "dp"),
            P(None, "dp", "tp"),
            P(None, "tp", None),
            P(None, "tp", None),
            P(None, "tp"),
            P(None, "tp", None, None),
            P(None, "tp", None, None),
            P(None, "tp", None, None),
            P(None, "tp", None, None),
            P(None, "tp"),
            P(None, "tp", "dp"),
            P(None, "tp", "dp"),
            P(None, "dp", "tp", None),
        ),
        out_specs=(P("tp", "dp"), P(None, "dp", "tp", None)),
        check_vma=False,
    )
```

```python
import functools

import jax
import jax.numpy as jnp
from jax import lax
from jax.experimental import pallas as pl
from jax.experimental.pallas import tpu as pltpu
from jax.sharding import PartitionSpec as P

EPS = 1e-06
F32 = jnp.float32
BF16 = jnp.bfloat16
HIGHEST = lax.Precision.HIGHEST
NT = (((1,), (1,)), ((), ()))


def partner(me, k, n, back=False):
    if n & (n - 1):
        return (me + (n - k if back else k)) % n
    found, bit = 0, 1
    while bit < n:
        mine = (me // bit) % 2
        found = found + (bit * (1 - mine) if k & bit else bit * mine)
        bit *= 2
    return found


def kernel(
    tp, dp, chans,
    stream_ref, gain_ref, w_in_hbm, lam_re_ref, lam_im_ref, log_dt_ref, b_re_hbm, b_im_hbm, c_re_hbm, c_im_hbm, skip_ref,
    w_val_hbm, w_gate_hbm, state_hbm,
    out_ref, state,
    w_in, w_val, w_gate, b_re, b_im, c_re, c_im, drive, read,
    kept, proj, u_keep, masked, from_old, mix_w,
    x_all, part_send, part_recv, sq_send, sq_recv, mix_all, block, comb_send, comb_own, pair_recv, comb_recv,
    load_sem, x_ss, x_rs, part_ss, part_rs, sq_ss, sq_rs, mix_ss, mix_rs, pair_ss, pair_rs, comb_ss, comb_rs,
):
    layers = w_in.shape[0]
    me_t, me_d = lax.axis_index("tp"), lax.axis_index("dp")
    rows_t, feats = stream_ref.shape
    rows_d, width = u_keep.shape[1:]
    per = rows_d // rows_t
    me_p, side = me_t // 2, me_t % 2
    groups, half = lam_re_ref.shape[1:]
    lanes = state.shape[2]
    sq_width = sq_send.shape[3]

    loads = {}
    for l in range(layers):
        for i, (src, dst) in enumerate(
            (
                (b_re_hbm, b_re), (b_im_hbm, b_im), (c_re_hbm, c_re), (c_im_hbm, c_im), (state_hbm, state),
                (w_in_hbm, w_in), (w_val_hbm, w_val), (w_gate_hbm, w_gate),
            )
        ):
            loads[l, i] = pltpu.make_async_copy(src.at[l], dst.at[l], load_sem.at[l, i])
            loads[l, i].start()

    barrier = pltpu.get_barrier_semaphore()
    for k in range(1, dp):
        pl.semaphore_signal(barrier, inc=1, device_id={"dp": partner(me_d, k, dp)}, device_id_type=pl.DeviceIdType.MESH)
    for k in range(1, tp):
        pl.semaphore_signal(barrier, inc=1, device_id={"tp": partner(me_t, k, tp)}, device_id_type=pl.DeviceIdType.MESH)

    def send(src, dst, ss, rs, axis, to):
        return pltpu.make_async_remote_copy(
            src_ref=src, dst_ref=dst, send_sem=ss, recv_sem=rs, device_id={axis: to}, device_id_type=pl.DeviceIdType.MESH
        )

    def x_copy(l, k):
        src = stream_ref if l == 0 else x_all.at[l, me_t]
        to = partner(me_t, k, tp)
        return send(src, x_all.at[l, me_t], x_ss.at[l, to], x_rs.at[l, me_t], "tp", to)

    def part_copy(l, to):
        return send(part_send.at[l, to], part_recv.at[l, me_d], part_ss.at[l, to], part_rs.at[l, me_d], "dp", to)

    def sq_copy(l, to):
        return send(sq_send.at[l, to], sq_recv.at[l, me_d], sq_ss.at[l, to], sq_rs.at[l, me_d], "dp", to)

    def mix_copy(l, to):
        return send(mix_all.at[l, me_d], mix_all.at[l, me_d], mix_ss.at[l, to], mix_rs.at[l, me_d], "dp", to)

    def comb_copy(l, to):
        return send(
            comb_send.at[l, 2 * to + side], comb_recv.at[l, me_p], comb_ss.at[l, to], comb_rs.at[l, me_p], "tp", 2 * to + side
        )

    def pair_copy(l, q):
        return send(
            comb_send.at[l, 2 * q + 1 - side], pair_recv.at[l, q], pair_ss.at[l, q], pair_rs.at[l, q], "tp", 2 * me_p + 1 - side
        )

    def arrival(ref, rs, axis):
        return send(ref, ref, rs, rs, axis, 0)

    lane_group = lax.broadcasted_iota(jnp.int32, (rows_d, width), 1) // chans
    eye = lax.broadcasted_iota(jnp.int32, (rows_d, sq_width), 0) == lax.broadcasted_iota(jnp.int32, (rows_d, sq_width), 1)

    group_eye = lax.broadcasted_iota(jnp.int32, (groups, groups), 0) == lax.broadcasted_iota(jnp.int32, (groups, groups), 1)

    def prepare(l):
        step_size = jnp.exp(jnp.sum(jnp.where(group_eye, log_dt_ref[l : l + 1, :], 0.0), axis=1, keepdims=True))
        lam_re, lam_im = lam_re_ref[l], lam_im_ref[l]
        decay = jnp.exp(lam_re * step_size)
        angle = lam_im * step_size
        keep_re = decay * jnp.cos(angle)
        keep_im = decay * jnp.sin(angle)
        denom = lam_re * lam_re + lam_im * lam_im
        ratio_re = ((keep_re - 1.0) * lam_re + keep_im * lam_im) / denom
        ratio_im = (keep_im * lam_re - (keep_re - 1.0) * lam_im) / denom
        keep_a = jnp.concatenate([keep_re, keep_re], axis=1)
        keep_b = jnp.concatenate([-keep_im, keep_im], axis=1)
        for i in range(5):
            loads[l, i].wait()
        for g in range(groups):
            t_re, t_im = b_re[l, g], b_im[l, g]
            r_re, r_im = ratio_re[g : g + 1, :], ratio_im[g : g + 1, :]
            drive[l, pl.ds(g * chans, chans), :] = jnp.concatenate(
                [r_re * t_re - r_im * t_im, r_re * t_im + r_im * t_re], axis=1
            )
        read[l] = jnp.concatenate([c_re[l].reshape(width, half), -c_im[l].reshape(width, half)], axis=1)
        for g in range(groups):
            old = state[l, pl.ds(g, rows_d, stride=groups), :]
            kept[l, pl.ds(g * rows_d, rows_d), :] = (
                keep_a[g : g + 1, :] * old + keep_b[g : g + 1, :] * pltpu.roll(old, lanes // 2, 1)
            )
        proj[...] = lax.dot_general(kept[l], read[l], NT, precision=HIGHEST, preferred_element_type=F32)
        total = jnp.zeros((rows_d, width), F32)
        for g in range(groups):
            total = jnp.where(lane_group == g, proj[pl.ds(g * rows_d, rows_d), :], total)
        from_old[l] = total
        full = lax.dot_general(drive[l], read[l], NT, precision=HIGHEST, preferred_element_type=F32)
        same = (
            lax.broadcasted_iota(jnp.int32, (width, width), 0) // chans
            == lax.broadcasted_iota(jnp.int32, (width, width), 1) // chans
        )
        mix_w[l] = jnp.where(same, full, 0.0)

    def update(l):
        u = u_keep[l]
        for g in range(groups):
            masked[pl.ds(g * rows_d, rows_d), :] = jnp.where(lane_group == g, u, 0.0)
        kept[l] = kept[l] + jnp.dot(masked[...], drive[l], precision=HIGHEST, preferred_element_type=F32)
        for g in range(groups):
            state[l, pl.ds(g, rows_d, stride=groups), :] = kept[l, pl.ds(g * rows_d, rows_d), :]

    pl.semaphore_wait(barrier, tp + dp - 2)
    for k in reversed(range(1, tp)):
        x_copy(0, k).start()
    x_all[0, me_t] = stream_ref[...]
    prepare(0)

    for l in range(layers):
        loads[l, 5].wait()
        gain = gain_ref[l : l + 1, :]
        own_part = own_sq = None
        for k in reversed(range(dp)):
            to = partner(me_d, k, dp)
            for j in range(per):
                t = to * per + j

                @pl.when(t != me_t)
                def _():
                    arrival(x_all.at[l, t], x_rs.at[l, t], "tp").wait_recv()

            x = x_all[l, pl.ds(to * per, per)].astype(F32).reshape(rows_d, feats)
            column = jnp.sum(x * x, axis=1, keepdims=True)
            squares = jnp.sum(jnp.where(eye, column, 0.0), axis=0, keepdims=True)
            product = jnp.dot((x * gain).astype(BF16), w_in[l], preferred_element_type=F32)
            if k:
                sq_send[l, to] = jnp.broadcast_to(squares, (8, sq_width))
                sq_copy(l, to).start()
                part_send[l, to] = product.astype(BF16)
                part_copy(l, to).start()
            else:
                own_part, own_sq = product, squares
        for k in range(1, dp):
            by = partner(me_d, k, dp, True)
            arrival(sq_recv.at[l, by], sq_rs.at[l, by], "dp").wait_recv()
            own_sq = own_sq + sq_recv[l, by][0:1, :]
            arrival(part_recv.at[l, by], part_rs.at[l, by], "dp").wait_recv()
            own_part = own_part + part_recv[l, by].astype(F32)
        square_total = jnp.sum(jnp.where(eye, own_sq, 0.0), axis=1, keepdims=True)
        u = lax.rsqrt(square_total / (feats * dp) + EPS) * own_part
        u_keep[l] = u
        pre = from_old[l] + jnp.dot(u, mix_w[l], precision=HIGHEST, preferred_element_type=F32) + skip_ref[l : l + 1, :] * u
        mix_all[l, me_d] = jax.nn.gelu(pre).astype(BF16)
        for k in reversed(range(1, dp)):
            mix_copy(l, partner(me_d, k, dp)).start()
        loads[l, 6].wait()
        loads[l, 7].wait()

        def pass_on(by):
            for m in range(per // 2):
                q = by * (per // 2) + m
                arrival(pair_recv.at[l, q], pair_rs.at[l, q], "tp").wait_recv()
                total = block[2 * q + side] + pair_recv[l, q].astype(F32)

                @pl.when(q != me_p)
                def _():
                    comb_send[l, 2 * q + side] = total.astype(BF16)
                    comb_copy(l, q).start()

                @pl.when(q == me_p)
                def _():
                    comb_own[...] = total

        for k in range(dp):
            by = partner(me_d, k, dp, True)
            if k:
                arrival(mix_all.at[l, by], mix_rs.at[l, by], "dp").wait_recv()
            mixed = mix_all[l, by]
            value = jnp.dot(mixed, w_val[l], preferred_element_type=F32)
            gate = jnp.dot(mixed, w_gate[l], preferred_element_type=F32)
            for j in range(per):
                rows = slice(j * rows_t, (j + 1) * rows_t)
                block[by * per + j, :, :feats] = value[rows]
                block[by * per + j, :, feats:] = gate[rows]
            for m in range(per // 2):
                q = by * (per // 2) + m
                comb_send[l, 2 * q + 1 - side] = block[2 * q + 1 - side].astype(BF16)
                pair_copy(l, q).start()
            if k:
                pass_on(partner(me_d, k - 1, dp, True))
        pass_on(partner(me_d, dp - 1, dp, True))

        update(l)
        if l + 1 < layers:
            prepare(l + 1)
        combined = comb_own[...]
        for k in range(1, tp // 2):
            by = partner(me_p, k, tp // 2, True)
            arrival(comb_recv.at[l, by], comb_rs.at[l, by], "tp").wait_recv()
            combined = combined + comb_recv[l, by].astype(F32)
        fresh = (
            x_all[l, me_t].astype(F32) + combined[:, :feats] * jax.nn.sigmoid(combined[:, feats:])
        ).astype(BF16)
        if l + 1 < layers:
            x_all[l + 1, me_t] = fresh
            for k in reversed(range(1, tp)):
                x_copy(l + 1, k).start()
        else:
            out_ref[...] = fresh

    for l in range(layers):
        for k in range(1, tp):
            x_copy(l, k).wait_send()
        for k in range(1, tp // 2):
            comb_copy(l, partner(me_p, k, tp // 2)).wait_send()
        for q in range(tp // 2):
            pair_copy(l, q).wait_send()
        for k in range(1, dp):
            to = partner(me_d, k, dp)
            part_copy(l, to).wait_send()
            sq_copy(l, to).wait_send()
            mix_copy(l, to).wait_send()


def per_device(
    tp, dp,
    stream, norm_gain, w_input, lam_re, lam_im, log_dt, b_re, b_im, readout_real, readout_imaginary, d_skip,
    w_val, w_gate, state,
):
    layers, feats, width = w_input.shape
    rows_t = stream.shape[0]
    rows_d, groups, lanes = state.shape[1:]
    chans = b_re.shape[-1]

    turned_re, turned_im = b_re.swapaxes(2, 3), b_im.swapaxes(2, 3)

    limit = 67043328 - 4 * layers * rows_d * groups * lanes - (256 << 10)
    vmem = pl.BlockSpec(memory_space=pltpu.VMEM)
    hbm = pl.BlockSpec(memory_space=pltpu.HBM)
    sq_width = max(rows_d, 128)
    dma = lambda *shape: pltpu.SemaphoreType.DMA(shape)
    out, states = pl.pallas_call(
        functools.partial(kernel, tp, dp, chans),
        out_shape=(pltpu.VMEM(stream.shape, BF16), pltpu.VMEM((layers, rows_d * groups, lanes), F32)),
        in_specs=[vmem, vmem, hbm, vmem, vmem, vmem, hbm, hbm, hbm, hbm, vmem, hbm, hbm, hbm],
        out_specs=(vmem, vmem),
        scratch_shapes=[
            pltpu.VMEM(w_input.shape, BF16),
            pltpu.VMEM(w_val.shape, BF16),
            pltpu.VMEM(w_gate.shape, BF16),
            pltpu.VMEM(turned_re.shape, F32),
            pltpu.VMEM(turned_im.shape, F32),
            pltpu.VMEM(readout_real.shape, F32),
            pltpu.VMEM(readout_imaginary.shape, F32),
            pltpu.VMEM((layers, width, lanes), F32),
            pltpu.VMEM((layers, width, lanes), F32),
            pltpu.VMEM((layers, rows_d * groups, lanes), F32),
            pltpu.VMEM((rows_d * groups, width), F32),
            pltpu.VMEM((layers, rows_d, width), F32),
            pltpu.VMEM((rows_d * groups, width), F32),
            pltpu.VMEM((layers, rows_d, width), F32),
            pltpu.VMEM((layers, width, width), F32),
            pltpu.VMEM((layers, tp, rows_t, feats), BF16),
            pltpu.VMEM((layers, dp, rows_d, width), BF16),
            pltpu.VMEM((layers, dp, rows_d, width), BF16),
            pltpu.VMEM((layers, dp, 8, sq_width), F32),
            pltpu.VMEM((layers, dp, 8, sq_width), F32),
            pltpu.VMEM((layers, dp, rows_d, width), BF16),
            pltpu.VMEM((tp, rows_t, 2 * feats), F32),
            pltpu.VMEM((layers, tp, rows_t, 2 * feats), BF16),
            pltpu.VMEM((rows_t, 2 * feats), F32),
            pltpu.VMEM((layers, tp // 2, rows_t, 2 * feats), BF16),
            pltpu.VMEM((layers, tp // 2, rows_t, 2 * feats), BF16),
            dma(layers, 8),
            dma(layers, tp), dma(layers, tp),
            dma(layers, dp), dma(layers, dp),
            dma(layers, dp), dma(layers, dp),
            dma(layers, dp), dma(layers, dp),
            dma(layers, tp // 2), dma(layers, tp // 2),
            dma(layers, tp // 2), dma(layers, tp // 2),
        ],
        compiler_params=pltpu.CompilerParams(collective_id=0, has_side_effects=True, vmem_limit_bytes=limit),
    )(
        stream, norm_gain, w_input, lam_re, lam_im, log_dt, turned_re, turned_im, readout_real,
        readout_imaginary, d_skip, w_val, w_gate,
        state.reshape(layers, rows_d * groups, lanes),
    )
    return out, states.reshape(state.shape)


def solution(mesh):
    return jax.shard_map(
        functools.partial(per_device, mesh.shape["tp"], mesh.shape["dp"]),
        mesh=mesh,
        in_specs=(
            P("tp", "dp"),
            P(None, "dp"),
            P(None, "dp", "tp"),
            P(None, "tp", None),
            P(None, "tp", None),
            P(None, "tp"),
            P(None, "tp", None, None),
            P(None, "tp", None, None),
            P(None, "tp", None, None),
            P(None, "tp", None, None),
            P(None, "tp"),
            P(None, "tp", "dp"),
            P(None, "tp", "dp"),
            P(None, "dp", "tp", None),
        ),
        out_specs=(P("tp", "dp"), P(None, "dp", "tp", None)),
        check_vma=False,
    )
```

```python
import functools

import jax
import jax.numpy as jnp
from jax import lax
from jax.experimental import pallas as pl
from jax.experimental.pallas import tpu as pltpu
from jax.sharding import PartitionSpec as P

EPS = 1e-06
F32 = jnp.float32
BF16 = jnp.bfloat16
HIGHEST = lax.Precision.HIGHEST
NT = (((1,), (1,)), ((), ()))


def partner(me, k, n, back=False):
    if n & (n - 1):
        return (me + (n - k if back else k)) % n
    found, bit = 0, 1
    while bit < n:
        mine = (me // bit) % 2
        found = found + (bit * (1 - mine) if k & bit else bit * mine)
        bit *= 2
    return found


def kernel(
    tp, dp, chans,
    stream_ref, gain_ref, w_in_hbm, lam_re_ref, lam_im_ref, log_dt_ref, b_re_hbm, b_im_hbm, c_re_hbm, c_im_hbm, skip_ref,
    w_val_hbm, w_gate_hbm, state_hbm,
    out_ref, state,
    w_in, w_val, w_gate, b_re, b_im, c_re, c_im, drive, read,
    kept, proj, u_keep, masked, from_old, mix_w,
    x_all, part_send, part_recv, sq_send, sq_recv, mix_all, block, comb_send, comb_own, pair_recv, comb_recv,
    load_sem, x_ss, x_rs, part_ss, part_rs, sq_ss, sq_rs, mix_ss, mix_rs, pair_ss, pair_rs, comb_ss, comb_rs,
):
    layers = w_in.shape[0]
    me_t, me_d = lax.axis_index("tp"), lax.axis_index("dp")
    rows_t, feats = stream_ref.shape
    rows_d, width = u_keep.shape[1:]
    per = rows_d // rows_t
    me_p, side = me_t // 2, me_t % 2
    groups, half = lam_re_ref.shape[1:]
    lanes = state.shape[2]
    sq_width = sq_send.shape[3]

    loads = {}
    for l in range(layers):
        for i, (src, dst) in enumerate(
            (
                (b_re_hbm, b_re), (b_im_hbm, b_im), (c_re_hbm, c_re), (c_im_hbm, c_im), (state_hbm, state),
                (w_in_hbm, w_in), (w_val_hbm, w_val), (w_gate_hbm, w_gate),
            )
        ):
            loads[l, i] = pltpu.make_async_copy(src.at[l], dst.at[l], load_sem.at[l, i])
            loads[l, i].start()

    barrier = pltpu.get_barrier_semaphore()
    for k in range(1, dp):
        pl.semaphore_signal(barrier, inc=1, device_id={"dp": partner(me_d, k, dp)}, device_id_type=pl.DeviceIdType.MESH)
    for k in range(1, tp):
        pl.semaphore_signal(barrier, inc=1, device_id={"tp": partner(me_t, k, tp)}, device_id_type=pl.DeviceIdType.MESH)

    def send(src, dst, ss, rs, axis, to):
        return pltpu.make_async_remote_copy(
            src_ref=src, dst_ref=dst, send_sem=ss, recv_sem=rs, device_id={axis: to}, device_id_type=pl.DeviceIdType.MESH
        )

    def x_copy(l, k):
        src = stream_ref if l == 0 else x_all.at[l, me_t]
        to = partner(me_t, k, tp)
        return send(src, x_all.at[l, me_t], x_ss.at[l, to], x_rs.at[l, me_t], "tp", to)

    def part_copy(l, to):
        return send(part_send.at[l, to], part_recv.at[l, me_d], part_ss.at[l, to], part_rs.at[l, me_d], "dp", to)

    def sq_copy(l, to):
        return send(sq_send.at[l, to], sq_recv.at[l, me_d], sq_ss.at[l, to], sq_rs.at[l, me_d], "dp", to)

    def mix_copy(l, to):
        return send(mix_all.at[l, me_d], mix_all.at[l, me_d], mix_ss.at[l, to], mix_rs.at[l, me_d], "dp", to)

    def comb_copy(l, to):
        return send(
            comb_send.at[l, 2 * to + side], comb_recv.at[l, me_p], comb_ss.at[l, to], comb_rs.at[l, me_p], "tp", 2 * to + side
        )

    def pair_copy(l, q):
        return send(
            comb_send.at[l, 2 * q + 1 - side], pair_recv.at[l, q], pair_ss.at[l, q], pair_rs.at[l, q], "tp", 2 * me_p + 1 - side
        )

    def arrival(ref, rs, axis):
        return send(ref, ref, rs, rs, axis, 0)

    lane_group = lax.broadcasted_iota(jnp.int32, (rows_d, width), 1) // chans
    eye = lax.broadcasted_iota(jnp.int32, (rows_d, sq_width), 0) == lax.broadcasted_iota(jnp.int32, (rows_d, sq_width), 1)

    group_eye = lax.broadcasted_iota(jnp.int32, (groups, groups), 0) == lax.broadcasted_iota(jnp.int32, (groups, groups), 1)

    def prepare(l):
        step_size = jnp.exp(jnp.sum(jnp.where(group_eye, log_dt_ref[l : l + 1, :], 0.0), axis=1, keepdims=True))
        lam_re, lam_im = lam_re_ref[l], lam_im_ref[l]
        decay = jnp.exp(lam_re * step_size)
        angle = lam_im * step_size
        keep_re = decay * jnp.cos(angle)
        keep_im = decay * jnp.sin(angle)
        denom = lam_re * lam_re + lam_im * lam_im
        ratio_re = ((keep_re - 1.0) * lam_re + keep_im * lam_im) / denom
        ratio_im = (keep_im * lam_re - (keep_re - 1.0) * lam_im) / denom
        keep_a = jnp.concatenate([keep_re, keep_re], axis=1)
        keep_b = jnp.concatenate([-keep_im, keep_im], axis=1)
        for i in range(5):
            loads[l, i].wait()
        for g in range(groups):
            t_re, t_im = b_re[l, g], b_im[l, g]
            r_re, r_im = ratio_re[g : g + 1, :], ratio_im[g : g + 1, :]
            drive[l, pl.ds(g * chans, chans), :] = jnp.concatenate(
                [r_re * t_re - r_im * t_im, r_re * t_im + r_im * t_re], axis=1
            )
        read[l] = jnp.concatenate([c_re[l].reshape(width, half), -c_im[l].reshape(width, half)], axis=1)
        for g in range(groups):
            old = state[l, pl.ds(g, rows_d, stride=groups), :]
            kept[l, pl.ds(g * rows_d, rows_d), :] = (
                keep_a[g : g + 1, :] * old + keep_b[g : g + 1, :] * pltpu.roll(old, lanes // 2, 1)
            )
        proj[...] = lax.dot_general(kept[l], read[l], NT, precision=HIGHEST, preferred_element_type=F32)
        total = jnp.zeros((rows_d, width), F32)
        for g in range(groups):
            total = jnp.where(lane_group == g, proj[pl.ds(g * rows_d, rows_d), :], total)
        from_old[l] = total
        full = lax.dot_general(drive[l], read[l], NT, precision=HIGHEST, preferred_element_type=F32)
        same = (
            lax.broadcasted_iota(jnp.int32, (width, width), 0) // chans
            == lax.broadcasted_iota(jnp.int32, (width, width), 1) // chans
        )
        mix_w[l] = jnp.where(same, full, 0.0)

    def update(l):
        u = u_keep[l]
        for g in range(groups):
            masked[pl.ds(g * rows_d, rows_d), :] = jnp.where(lane_group == g, u, 0.0)
        kept[l] = kept[l] + jnp.dot(masked[...], drive[l], precision=HIGHEST, preferred_element_type=F32)
        for g in range(groups):
            state[l, pl.ds(g, rows_d, stride=groups), :] = kept[l, pl.ds(g * rows_d, rows_d), :]

    pl.semaphore_wait(barrier, tp + dp - 2)
    for k in reversed(range(1, tp)):
        x_copy(0, k).start()
    x_all[0, me_t] = stream_ref[...]
    prepare(0)

    for l in range(layers):
        loads[l, 5].wait()
        gain = gain_ref[l : l + 1, :]
        own_part = own_sq = None
        for k in reversed(range(dp)):
            to = partner(me_d, k, dp)
            for j in range(per):
                t = to * per + j

                @pl.when(t != me_t)
                def _():
                    arrival(x_all.at[l, t], x_rs.at[l, t], "tp").wait_recv()

            x = x_all[l, pl.ds(to * per, per)].astype(F32).reshape(rows_d, feats)
            column = jnp.sum(x * x, axis=1, keepdims=True)
            squares = jnp.sum(jnp.where(eye, column, 0.0), axis=0, keepdims=True)
            product = jnp.dot((x * gain).astype(BF16), w_in[l], preferred_element_type=F32)
            if k:
                sq_send[l, to] = jnp.broadcast_to(squares, (8, sq_width))
                sq_copy(l, to).start()
                part_send[l, to] = product.astype(BF16)
                part_copy(l, to).start()
            else:
                own_part, own_sq = product, squares
        for k in range(1, dp):
            by = partner(me_d, k, dp, True)
            arrival(sq_recv.at[l, by], sq_rs.at[l, by], "dp").wait_recv()
            own_sq = own_sq + sq_recv[l, by][0:1, :]
            arrival(part_recv.at[l, by], part_rs.at[l, by], "dp").wait_recv()
            own_part = own_part + part_recv[l, by].astype(F32)
        square_total = jnp.sum(jnp.where(eye, own_sq, 0.0), axis=1, keepdims=True)
        u = lax.rsqrt(square_total / (feats * dp) + EPS) * own_part
        u_keep[l] = u
        pre = from_old[l] + jnp.dot(u, mix_w[l], precision=HIGHEST, preferred_element_type=F32) + skip_ref[l : l + 1, :] * u
        mix_all[l, me_d] = jax.nn.gelu(pre).astype(BF16)
        for k in reversed(range(1, dp)):
            mix_copy(l, partner(me_d, k, dp)).start()
        loads[l, 6].wait()
        loads[l, 7].wait()

        def pass_on(by):
            for m in range(per // 2):
                q = by * (per // 2) + m
                arrival(pair_recv.at[l, q], pair_rs.at[l, q], "tp").wait_recv()
                total = block[2 * q + side] + pair_recv[l, q].astype(F32)

                @pl.when(q != me_p)
                def _():
                    comb_send[l, 2 * q + side] = total.astype(BF16)
                    comb_copy(l, q).start()

                @pl.when(q == me_p)
                def _():
                    comb_own[...] = total

        for k in range(dp):
            by = partner(me_d, k, dp, True)
            if k:
                arrival(mix_all.at[l, by], mix_rs.at[l, by], "dp").wait_recv()
            mixed = mix_all[l, by]
            value = jnp.dot(mixed, w_val[l], preferred_element_type=F32)
            gate = jnp.dot(mixed, w_gate[l], preferred_element_type=F32)
            for j in range(per):
                rows = slice(j * rows_t, (j + 1) * rows_t)
                block[by * per + j, :, :feats] = value[rows]
                block[by * per + j, :, feats:] = gate[rows]
            for m in range(per // 2):
                q = by * (per // 2) + m
                comb_send[l, 2 * q + 1 - side] = block[2 * q + 1 - side].astype(BF16)
                pair_copy(l, q).start()
            if k > 1:
                pass_on(partner(me_d, k - 2, dp, True))
        for k in range(max(dp - 2, 0), dp):
            pass_on(partner(me_d, k, dp, True))

        update(l)
        if l + 1 < layers:
            prepare(l + 1)
        combined = comb_own[...]
        for k in range(1, tp // 2):
            by = partner(me_p, k, tp // 2, True)
            arrival(comb_recv.at[l, by], comb_rs.at[l, by], "tp").wait_recv()
            combined = combined + comb_recv[l, by].astype(F32)
        fresh = (
            x_all[l, me_t].astype(F32) + combined[:, :feats] * jax.nn.sigmoid(combined[:, feats:])
        ).astype(BF16)
        if l + 1 < layers:
            x_all[l + 1, me_t] = fresh
            for k in reversed(range(1, tp)):
                x_copy(l + 1, k).start()
        else:
            out_ref[...] = fresh

    for l in range(layers):
        for k in range(1, tp):
            x_copy(l, k).wait_send()
        for k in range(1, tp // 2):
            comb_copy(l, partner(me_p, k, tp // 2)).wait_send()
        for q in range(tp // 2):
            pair_copy(l, q).wait_send()
        for k in range(1, dp):
            to = partner(me_d, k, dp)
            part_copy(l, to).wait_send()
            sq_copy(l, to).wait_send()
            mix_copy(l, to).wait_send()


def per_device(
    tp, dp,
    stream, norm_gain, w_input, lam_re, lam_im, log_dt, b_re, b_im, readout_real, readout_imaginary, d_skip,
    w_val, w_gate, state,
):
    layers, feats, width = w_input.shape
    rows_t = stream.shape[0]
    rows_d, groups, lanes = state.shape[1:]
    chans = b_re.shape[-1]

    turned_re, turned_im = b_re.swapaxes(2, 3), b_im.swapaxes(2, 3)

    limit = 67043328 - 4 * layers * rows_d * groups * lanes - (256 << 10)
    vmem = pl.BlockSpec(memory_space=pltpu.VMEM)
    hbm = pl.BlockSpec(memory_space=pltpu.HBM)
    sq_width = max(rows_d, 128)
    dma = lambda *shape: pltpu.SemaphoreType.DMA(shape)
    out, states = pl.pallas_call(
        functools.partial(kernel, tp, dp, chans),
        out_shape=(pltpu.VMEM(stream.shape, BF16), pltpu.VMEM((layers, rows_d * groups, lanes), F32)),
        in_specs=[vmem, vmem, hbm, vmem, vmem, vmem, hbm, hbm, hbm, hbm, vmem, hbm, hbm, hbm],
        out_specs=(vmem, vmem),
        scratch_shapes=[
            pltpu.VMEM(w_input.shape, BF16),
            pltpu.VMEM(w_val.shape, BF16),
            pltpu.VMEM(w_gate.shape, BF16),
            pltpu.VMEM(turned_re.shape, F32),
            pltpu.VMEM(turned_im.shape, F32),
            pltpu.VMEM(readout_real.shape, F32),
            pltpu.VMEM(readout_imaginary.shape, F32),
            pltpu.VMEM((layers, width, lanes), F32),
            pltpu.VMEM((layers, width, lanes), F32),
            pltpu.VMEM((layers, rows_d * groups, lanes), F32),
            pltpu.VMEM((rows_d * groups, width), F32),
            pltpu.VMEM((layers, rows_d, width), F32),
            pltpu.VMEM((rows_d * groups, width), F32),
            pltpu.VMEM((layers, rows_d, width), F32),
            pltpu.VMEM((layers, width, width), F32),
            pltpu.VMEM((layers, tp, rows_t, feats), BF16),
            pltpu.VMEM((layers, dp, rows_d, width), BF16),
            pltpu.VMEM((layers, dp, rows_d, width), BF16),
            pltpu.VMEM((layers, dp, 8, sq_width), F32),
            pltpu.VMEM((layers, dp, 8, sq_width), F32),
            pltpu.VMEM((layers, dp, rows_d, width), BF16),
            pltpu.VMEM((tp, rows_t, 2 * feats), F32),
            pltpu.VMEM((layers, tp, rows_t, 2 * feats), BF16),
            pltpu.VMEM((rows_t, 2 * feats), F32),
            pltpu.VMEM((layers, tp // 2, rows_t, 2 * feats), BF16),
            pltpu.VMEM((layers, tp // 2, rows_t, 2 * feats), BF16),
            dma(layers, 8),
            dma(layers, tp), dma(layers, tp),
            dma(layers, dp), dma(layers, dp),
            dma(layers, dp), dma(layers, dp),
            dma(layers, dp), dma(layers, dp),
            dma(layers, tp // 2), dma(layers, tp // 2),
            dma(layers, tp // 2), dma(layers, tp // 2),
        ],
        compiler_params=pltpu.CompilerParams(collective_id=0, has_side_effects=True, vmem_limit_bytes=limit),
    )(
        stream, norm_gain, w_input, lam_re, lam_im, log_dt, turned_re, turned_im, readout_real,
        readout_imaginary, d_skip, w_val, w_gate,
        state.reshape(layers, rows_d * groups, lanes),
    )
    return out, states.reshape(state.shape)


def solution(mesh):
    return jax.shard_map(
        functools.partial(per_device, mesh.shape["tp"], mesh.shape["dp"]),
        mesh=mesh,
        in_specs=(
            P("tp", "dp"),
            P(None, "dp"),
            P(None, "dp", "tp"),
            P(None, "tp", None),
            P(None, "tp", None),
            P(None, "tp"),
            P(None, "tp", None, None),
            P(None, "tp", None, None),
            P(None, "tp", None, None),
            P(None, "tp", None, None),
            P(None, "tp"),
            P(None, "tp", "dp"),
            P(None, "tp", "dp"),
            P(None, "dp", "tp", None),
        ),
        out_specs=(P("tp", "dp"), P(None, "dp", "tp", None)),
        check_vma=False,
    )
```
